32 devices in a mesh: sp: 8 (over z, x), tp: 4 (over y, core).
Axes of the slice: x: 2, y: 2, z: 4, core: 2. Of those that a mesh axis runs over, the one named last changes fastest.
Arguments:
- residual: bfloat16 [4096, 2048], P('sp'), may hold values from -6 to 6
- queries: bfloat16 [4096, 1024], P('sp', 'tp'), may hold values from -384 to 384
- key_pairs: bfloat16 [4096, 1024], P('sp', 'tp'), may hold values from -384 to 384
- values: bfloat16 [4096, 1024], P('sp', 'tp'), may hold values from -6 to 6
- lambdas: float32 [8], P('tp'), may hold values from 0.3 to 0.8
- head_gain: float32 [128], replicated, may hold values from 0.1 to 1.9
- w_out: bfloat16 [1024, 2048], replicated, may hold values from -0.1875 to 0.1875
- norm_gain: float32 [2048], replicated, may hold values from 0.1 to 1.9
- w_gate: bfloat16 [2048, 5632], P('sp', 'tp'), may hold values from -0.125 to 0.125
- w_up: bfloat16 [2048, 5632], P('sp', 'tp'), may hold values from -0.125 to 0.125
- w_down: bfloat16 [5632, 2048], P('tp', 'sp'), may hold values from -0.078125 to 0.078125
Outputs:
- layer_out: bfloat16 [4096, 2048], P(('sp', 'tp'))
The draws below stay inside these ranges and needn't reach their ends.
All inputs are finite; a program needn't handle non-finite values.
Results may differ from the reference program's by a relative error of at most 0.018.
Values may be sent and summed in bfloat16 or wider, within the bound.
A program may use at most 128 MiB of HBM per device.

```python
import math
import jax
import jax.numpy as jnp
from jax import lax

D = 2048
HEADS = 8
HD = 64
VD = 128
FF = 5632
SEQ = 4096
N_TP = 4


def drawn_pair(key):
    query_key, pair_key = jax.random.split(jax.random.fold_in(key, 11), 2)
    query_draw = jnp.clip(jax.random.normal(query_key, (SEQ, HEADS, 2, HD), jnp.float32), -6.0, 6.0) * 1.3
    key_draw = jnp.clip(jax.random.normal(pair_key, (SEQ, HEADS, 2, HD), jnp.float32), -6.0, 6.0) * 1.3
    return (query_draw.reshape(SEQ, HEADS * 2 * HD), key_draw.reshape(SEQ, HEADS * 2 * HD))


def draw_queries(key, part):
    return drawn_pair(key)[0].astype(jnp.bfloat16)


def draw_key_pairs(key, part):
    return drawn_pair(key)[1].astype(jnp.bfloat16)


def shard_levels(rng, dims, cuts, low, top_value):
    def one(position, blocks):
        draws = jax.random.uniform(jax.random.fold_in(jax.random.fold_in(rng, 6), position), (blocks,), jnp.float32, low / len(cuts), top_value / len(cuts))
        return jnp.repeat(jnp.exp(draws), dims[position] // blocks).reshape((-1,) + (1,) * (len(dims) - position - 1))

    factor_of = one(*cuts[0])
    for cut in cuts[1:]:
        factor_of = factor_of * one(*cut)
    return factor_of


def scatter_about(own_key, shape, deviation, bound, cuts=(), kind=jnp.bfloat16):
    loudness = shard_levels(own_key, shape, cuts, -0.22, 0.18) if cuts else 1.0
    result = jax.random.normal(own_key, shape, jnp.float32) * deviation * loudness
    return jnp.minimum(jnp.maximum(result, -bound), bound).astype(kind)


def setup_inputs(seed: int = 0) -> dict:
    arg_keys = jax.random.split(jax.random.key(seed), 12)
    residual = scatter_about(arg_keys[0], (SEQ, D), 1.0, 6.0, ((0, 8),))
    queries = draw_queries(jax.random.fold_in(arg_keys[11], 71), 0)
    key_pairs = draw_key_pairs(jax.random.fold_in(arg_keys[11], 71), 0)
    values = scatter_about(arg_keys[3], (SEQ, HEADS * VD), 1.0, 6.0, ((0, 8), (1, 4)))
    lambdas = jnp.clip(0.3 + 0.5 * jax.random.uniform(arg_keys[4], (HEADS,), jnp.float32) ** shard_levels(arg_keys[4], (HEADS,), ((0, 4),), -0.2, 0.2), 0.3, 0.8)
    head_gain = jnp.clip(1.0 + 0.18 * jax.random.normal(arg_keys[5], (VD,), jnp.float32), 0.1, 1.9)
    w_out = scatter_about(arg_keys[6], (HEADS * VD, D), (HEADS * VD) ** -0.5, 0.1875)
    norm_gain = jnp.clip(1.0 + 0.18 * jax.random.normal(arg_keys[7], (D,), jnp.float32), 0.1, 1.9)
    w_gate = scatter_about(arg_keys[8], (D, FF), D ** -0.5, 0.125, ((0, 8), (1, 4)))
    w_up = scatter_about(arg_keys[9], (D, FF), D ** -0.5, 0.125, ((0, 8), (1, 4)))
    w_down = scatter_about(arg_keys[10], (FF, D), FF ** -0.5, 0.078125, ((0, 4), (1, 8)))
    return {"residual": residual, "queries": queries, "key_pairs": key_pairs, "values": values, "lambdas": lambdas, "head_gain": head_gain, "w_out": w_out, "norm_gain": norm_gain, "w_gate": w_gate, "w_up": w_up, "w_down": w_down}


def reference(residual, queries, key_pairs, values, lambdas, head_gain, w_out, norm_gain, w_gate, w_up, w_down):
    score_scale = HD ** (-0.5)
    value_width = 2 * HD
    key_all = key_pairs.reshape(SEQ, HEADS, 2, HD).astype(jnp.float32)
    value_all = values.reshape(SEQ, HEADS, value_width).astype(jnp.float32)
    query_rows = math.gcd(SEQ, 256)

    def attend(query_block):
        scores = jnp.einsum('qhmd,khmd->hmqk', query_block.astype(jnp.float32), key_all) * score_scale
        highest = lax.optimization_barrier(jnp.max(scores, axis=-1, keepdims=True))
        weights = jnp.exp(scores - highest)
        totals = lax.optimization_barrier(jnp.sum(weights, axis=-1))
        rounded = lax.optimization_barrier(weights.astype(jnp.bfloat16)).astype(jnp.float32)
        mixture = jnp.einsum('hmqk,khe->hmqe', rounded, value_all) / totals[..., None]
        differ = mixture[:, 0] - lambdas[:, None, None] * mixture[:, 1]
        normed_heads = differ * lax.rsqrt(lax.optimization_barrier(jnp.mean(differ * differ, axis=-1, keepdims=True)) + 1e-05) * head_gain
        return jnp.transpose(normed_heads, (1, 0, 2)).reshape(query_rows, HEADS * value_width).astype(jnp.bfloat16)
    query_blocks = queries.reshape(SEQ // query_rows, query_rows, HEADS, 2, HD)
    heads_out = lax.map(attend, query_blocks).reshape(SEQ, HEADS * value_width)
    projected = jnp.dot(heads_out, w_out, preferred_element_type=jnp.float32)
    hidden_state = (residual.astype(jnp.float32) + projected).astype(jnp.bfloat16)
    stream_f = hidden_state.astype(jnp.float32)
    normed = (stream_f * lax.rsqrt(lax.optimization_barrier(jnp.mean(stream_f * stream_f, axis=-1, keepdims=True)) + 1e-05) * norm_gain).astype(jnp.bfloat16)
    group_width = FF // N_TP
    summed = jnp.zeros((SEQ, D), jnp.float32)
    for member in range(N_TP):
        lower = member * group_width
        gate_part = jnp.dot(normed, w_gate[:, lower:lower + group_width], preferred_element_type=jnp.float32)
        up_part = jnp.dot(normed, w_up[:, lower:lower + group_width], preferred_element_type=jnp.float32)
        hidden_part = (jax.nn.silu(gate_part) * up_part).astype(jnp.bfloat16)
        partial_sum = jnp.dot(hidden_part, w_down[lower:lower + group_width], preferred_element_type=jnp.float32)
        summed = summed + lax.optimization_barrier(partial_sum.astype(jnp.bfloat16)).astype(jnp.float32)
    return (stream_f + summed).astype(jnp.bfloat16)
```

```python
import functools

import jax
import jax.numpy as jnp
import numpy as np
from jax import lax
from jax.experimental import pallas as pl
from jax.experimental.pallas import tpu as pltpu
from jax.sharding import Mesh, PartitionSpec as P

HD = 64


def attend_chunk(q, k, v, m_ref, l_ref, acc_ref, slot, rows):
    scores = lax.dot_general(
        q, k, (((1,), (1,)), ((), ())), preferred_element_type=jnp.float32
    )
    old = m_ref[slot, rows, :]
    high = jnp.maximum(old, jnp.max(scores, axis=1, keepdims=True))
    shrink = jnp.exp(old - high)
    weights = jnp.exp(scores - high[:, :1])
    l_ref[slot, rows, :] = l_ref[slot, rows, :] * shrink + jnp.sum(weights, axis=1, keepdims=True)
    m_ref[slot, rows, :] = high
    acc_ref[slot, rows, :] = acc_ref[slot, rows, :] * shrink + jnp.dot(
        weights.astype(jnp.bfloat16), v, preferred_element_type=jnp.float32
    )


def finish_heads(heads, width, lam_ref, gain_ref, l_ref, acc_ref, out_ref):
    for h in range(heads):
        first = acc_ref[2 * h] / l_ref[2 * h]
        second = acc_ref[2 * h + 1] / l_ref[2 * h + 1]
        differ = first - lam_ref[h] * second
        scale = lax.rsqrt(jnp.mean(differ * differ, axis=1, keepdims=True) + 1e-05)
        out_ref[:, h * width : (h + 1) * width] = (differ * scale * gain_ref[...]).astype(out_ref.dtype)


def attention_kernel(heads, chunk, block, lam_ref, q_ref, kv_ref, gain_ref, out_ref, m_ref, l_ref, acc_ref):
    rows_all = q_ref.shape[0]
    width = out_ref.shape[1] // heads
    keys = heads * 2 * HD
    m_ref[...] = jnp.full_like(m_ref, -jnp.inf)
    l_ref[...] = jnp.zeros_like(l_ref)
    acc_ref[...] = jnp.zeros_like(acc_ref)

    def step(i, _):
        part = pl.ds(pl.multiple_of(i * chunk, chunk), chunk)
        for h in range(heads):
            v = kv_ref[part, keys + h * width : keys + (h + 1) * width]
            for m in range(2):
                lane = (2 * h + m) * HD
                k = kv_ref[part, lane : lane + HD]
                for r in range(0, rows_all, block):
                    rows = pl.ds(r, block)
                    q = q_ref[rows, lane : lane + HD] * jnp.bfloat16(HD**-0.5)
                    attend_chunk(q, k, v, m_ref, l_ref, acc_ref, 2 * h + m, rows)
        return 0

    lax.fori_loop(0, kv_ref.shape[0] // chunk, step, 0)
    finish_heads(heads, width, lam_ref, gain_ref, l_ref, acc_ref, out_ref)


def attention(queries, kv, lambdas, head_gain):
    rows = queries.shape[0]
    heads = lambdas.shape[0]
    width = head_gain.shape[0]
    vmem = pl.BlockSpec(memory_space=pltpu.VMEM)
    return pl.pallas_call(
        functools.partial(attention_kernel, heads, 512, 256),
        out_shape=jax.ShapeDtypeStruct((rows, heads * width), jnp.bfloat16),
        in_specs=[pl.BlockSpec(memory_space=pltpu.SMEM), vmem, vmem, vmem],
        out_specs=vmem,
        scratch_shapes=[pltpu.VMEM((2 * heads, rows, width), jnp.float32)] * 3,
        cost_estimate=pl.CostEstimate(
            flops=rows * kv.shape[0] * heads * 1024, bytes_accessed=4000000, transcendentals=0
        ),
        name="attend",
    )(lambdas, queries, kv, head_gain.reshape(1, width))


def exchange(block, nz, nx):
    me = lax.axis_index("z")
    pieces = [lax.dynamic_index_in_dim(block, me, 0, keepdims=False)]
    slots = [me]
    for d in range(1, nz):
        piece = lax.dynamic_index_in_dim(block, lax.rem(me + d, nz), 0, keepdims=False)
        pieces.append(lax.ppermute(piece, "z", [(i, (i + d) % nz) for i in range(nz)]))
        slots.append(lax.rem(me - d + nz, nz))
    x = lax.axis_index("x")
    out = jnp.zeros((nz, nx) + block.shape[1:], block.dtype)
    for piece, slot in zip(pieces, slots):
        for e in range(nx):
            got = piece if e == 0 else lax.ppermute(piece, "x", [(i, (i + e) % nx) for i in range(nx)])
            out = lax.dynamic_update_slice(
                out, got[None, None], (slot, lax.rem(x - e + nx, nx)) + (0,) * (block.ndim - 1)
            )
    return out


def per_device(
    nz, nx, residual, queries, key_pairs, values, lambdas, head_gain, w_out, norm_gain, w_gate, w_up, w_down
):
    local_rows = queries.shape[0]
    heads_here = lambdas.shape[0]
    value_width = head_gain.shape[0]
    d_rows, units = w_gate.shape
    mine = units // nz
    width = residual.shape[1]

    kv = lax.all_gather(jnp.concatenate([key_pairs, values], axis=1), ("z", "x"), axis=0, tiled=True)
    joined = jnp.stack([w_gate.reshape(d_rows, nz, mine), w_up.reshape(d_rows, nz, mine)], axis=2)
    joined = jnp.transpose(joined, (1, 2, 0, 3))
    both = exchange(joined, nz, nx)
    down = exchange(w_down.reshape(nz, mine, w_down.shape[1]), nz, nx)
    gate = jnp.transpose(both[:, :, 0], (0, 1, 2, 3)).reshape(width, mine)
    up = both[:, :, 1].reshape(width, mine)
    down = jnp.transpose(down, (2, 0, 1, 3)).reshape(mine, width)

    heads_out = attention(queries, kv, lambdas, head_gain)
    tp_index = lax.axis_index("tp")
    own_rows = local_rows // lax.axis_size("tp")
    w_mine = lax.dynamic_slice_in_dim(
        w_out, tp_index * heads_here * value_width, heads_here * value_width, 0
    )
    projected = lax.psum_scatter(
        jnp.dot(heads_out, w_mine, preferred_element_type=jnp.float32).astype(jnp.bfloat16),
        "tp",
        scatter_dimension=0,
        tiled=True,
    ).astype(jnp.float32)
    residual_own = lax.dynamic_slice_in_dim(residual, tp_index * own_rows, own_rows, 0)
    hidden_own = (residual_own.astype(jnp.float32) + projected).astype(jnp.bfloat16)
    stream_f = hidden_own.astype(jnp.float32)
    scaled = stream_f * lax.rsqrt(jnp.mean(stream_f * stream_f, axis=-1, keepdims=True) + 1e-05)
    normed_rows = lax.all_gather(
        (scaled * norm_gain).astype(jnp.bfloat16), ("z", "tp"), axis=0, tiled=True
    )
    gate_sum = jnp.dot(normed_rows, gate, preferred_element_type=jnp.float32)
    up_sum = jnp.dot(normed_rows, up, preferred_element_type=jnp.float32)
    hidden_units = (jax.nn.silu(gate_sum) * up_sum).astype(jnp.bfloat16)
    ffn_out = lax.psum_scatter(
        jnp.dot(hidden_units, down, preferred_element_type=jnp.float32).astype(jnp.bfloat16),
        ("z", "tp"),
        scatter_dimension=0,
        tiled=True,
    ).astype(jnp.float32)
    return (hidden_own.astype(jnp.float32) + ffn_out).astype(jnp.bfloat16)


def solution(mesh):
    sp, tp = mesh.shape["sp"], mesh.shape["tp"]
    coords = [getattr(d, "coords", None) for d in mesh.devices.flat]
    nx = len({c[0] for c in coords}) if all(c is not None for c in coords) else 2
    if sp % nx:
        nx = 1
    nz = sp // nx
    cube = Mesh(np.asarray(mesh.devices).reshape(nz, nx, tp), ("z", "x", "tp"))
    zx = ("z", "x")
    placed = (
        P(zx, None),
        P(zx, "tp"),
        P(zx, "tp"),
        P(zx, "tp"),
        P("tp"),
        P(),
        P(),
        P(),
        P(zx, "tp"),
        P(zx, "tp"),
        P("tp", zx),
    )
    return jax.shard_map(
        functools.partial(per_device, nz, nx),
        mesh=cube,
        in_specs=placed,
        out_specs=P(("z", "x", "tp"), None),
        check_vma=False,
    )
```

```python
import functools

import jax
import jax.numpy as jnp
import numpy as np
from jax import lax
from jax.experimental import pallas as pl
from jax.experimental.pallas import tpu as pltpu
from jax.sharding import Mesh, PartitionSpec as P

HD = 64


def attend_chunk(q, k, v, m_ref, l_ref, acc_ref, slot, rows):
    scores = lax.dot_general(
        q, k, (((1,), (1,)), ((), ())), preferred_element_type=jnp.float32
    )
    old = m_ref[slot, rows, :]
    high = jnp.maximum(old, jnp.max(scores, axis=1, keepdims=True))
    shrink = jnp.exp(old - high)
    weights = jnp.exp(scores - high[:, :1])
    l_ref[slot, rows, :] = l_ref[slot, rows, :] * shrink + jnp.sum(weights, axis=1, keepdims=True)
    m_ref[slot, rows, :] = high
    acc_ref[slot, rows, :] = acc_ref[slot, rows, :] * shrink + jnp.dot(
        weights.astype(jnp.bfloat16), v, preferred_element_type=jnp.float32
    )


def finish_heads(heads, width, lam_ref, gain_ref, l_ref, acc_ref, out_ref):
    for h in range(heads):
        first = acc_ref[2 * h] / l_ref[2 * h]
        second = acc_ref[2 * h + 1] / l_ref[2 * h + 1]
        differ = first - lam_ref[h] * second
        scale = lax.rsqrt(jnp.mean(differ * differ, axis=1, keepdims=True) + 1e-05)
        out_ref[:, h * width : (h + 1) * width] = (differ * scale * gain_ref[...]).astype(out_ref.dtype)


def nearest(k, me, n):
    low, high = me, n - 1 - me
    edge = jnp.minimum(low, high)
    side = jnp.where(high >= low, 1, -1)
    near = jnp.where(k % 2 == 1, 1, -1) * ((k + 1) // 2)
    off = side * jnp.where(k <= 2 * edge, near, k - edge)
    return me + off, off


def gather_attend_kernel(
    nz, nx, heads, block,
    lam_ref, q_ref, kv_ref, gain_ref, pair_ref, down_ref,
    out_ref, pair_out, down_out,
    kv_all, m_ref, l_ref, acc_ref,
    up_sem, low_sem, side_sem, kv_sem, pz_sem, dz_sem, px_sem, dx_sem, p_sem, d_sem,
):
    z, x = lax.axis_index("z"), lax.axis_index("x")
    rows_all = q_ref.shape[0]
    width = out_ref.shape[1] // heads
    keys = heads * 2 * HD
    depth = pair_ref.shape[2]

    def remote(src, dst, send, recv, zz, xx):
        return pltpu.make_async_remote_copy(
            src_ref=src, dst_ref=dst, send_sem=send, recv_sem=recv,
            device_id={"z": zz, "x": xx}, device_id_type=pl.DeviceIdType.MESH,
        )

    barrier = pltpu.get_barrier_semaphore()
    for a in range(nz):
        for b in range(nx):
            if a + b > 0:
                pl.semaphore_signal(
                    barrier, inc=1,
                    device_id={"z": lax.rem(z + a, nz), "x": lax.rem(x + b, nx)},
                    device_id_type=pl.DeviceIdType.MESH,
                )
    pl.semaphore_wait(barrier, nz * nx - 1)

    def slot(zz, xx):
        return zz * nx + xx

    def flow(src, k, zz, go):
        off = zz - z
        here = kv_all.at[slot(zz, x)]

        @pl.when(jnp.logical_and(off <= 0, z < nz - 1))
        def _():
            go(remote(src, here, up_sem.at[k], kv_sem.at[slot(zz, x)], jnp.minimum(z + 1, nz - 1), x))

        @pl.when(jnp.logical_and(off >= 0, z > 0))
        def _():
            go(remote(src, here, low_sem.at[k], kv_sem.at[slot(zz, x)], jnp.maximum(z - 1, 0), x))

        for e in range(1, nx):
            go(remote(src, here, side_sem.at[e - 1, k], kv_sem.at[slot(zz, x)], z, lax.rem(x + e, nx)))

    def pair_place(s):
        return pair_out.at[:, pl.ds(pl.multiple_of(s * depth, depth), depth), :]

    def along(d, go):
        to = lax.rem(z + d, nz)
        s = slot(z, x)
        go(remote(pair_ref.at[to], pair_place(s), pz_sem.at[d], p_sem.at[s], to, x))
        go(remote(down_ref.at[to], down_out.at[s], dz_sem.at[d], d_sem.at[s], to, x))

    def across(src_pair, src_down, d, s, go):
        for e in range(1, nx):
            to = lax.rem(x + e, nx)
            go(remote(src_pair, pair_place(s), px_sem.at[e - 1, d], p_sem.at[s], z, to))
            go(remote(src_down, down_out.at[s], dx_sem.at[e - 1, d], d_sem.at[s], z, to))

    def arrived(src_pair, src_down, s):
        remote(src_pair, pair_place(s), pz_sem.at[0], p_sem.at[s], z, x).wait_recv()
        remote(src_down, down_out.at[s], dz_sem.at[0], d_sem.at[s], z, x).wait_recv()

    start = lambda copy: copy.start()
    sent = lambda copy: copy.wait_send()

    flow(kv_ref, 0, z, start)
    mine = slot(z, x)
    pair_out[:, pl.ds(pl.multiple_of(mine * depth, depth), depth), :] = pair_ref[z]
    down_out[mine] = down_ref[z]
    kv_all[mine] = kv_ref[...]
    m_ref[...] = jnp.full_like(m_ref, -jnp.inf)
    l_ref[...] = jnp.zeros_like(l_ref)
    acc_ref[...] = jnp.zeros_like(acc_ref)

    def attend(s):
        for h in range(heads):
            v = kv_all[s, :, keys + h * width : keys + (h + 1) * width]
            for m in range(2):
                lane = (2 * h + m) * HD
                k = kv_all[s, :, lane : lane + HD]
                for r in range(0, rows_all, block):
                    rows = pl.ds(r, block)
                    q = q_ref[rows, lane : lane + HD] * jnp.bfloat16(HD**-0.5)
                    attend_chunk(q, k, v, m_ref, l_ref, acc_ref, 2 * h + m, rows)

    def step(k, _):
        zz, _off = nearest(k, z, nz)
        here = kv_all.at[slot(zz, x)]

        @pl.when(k > 0)
        def _():
            remote(kv_ref, here, up_sem.at[k], kv_sem.at[slot(zz, x)], z, x).wait_recv()
            flow(here, k, zz, start)

        @pl.when(k == min(1, nz - 1))
        def _():
            for d in range(1, nz):
                along(d, start)
            across(pair_ref.at[z], down_ref.at[z], 0, mine, start)

        def column(e, _):
            other = lax.rem(x - e + nx, nx)

            @pl.when(e > 0)
            def _():
                remote(kv_ref, here, up_sem.at[k], kv_sem.at[slot(zz, other)], z, x).wait_recv()

            attend(slot(zz, other))
            return 0

        lax.fori_loop(0, nx, column, 0)
        return 0

    lax.fori_loop(0, nz, step, 0)
    for d in range(1, nz):
        zz = lax.rem(z - d + nz, nz)
        s = slot(zz, x)
        arrived(pair_ref.at[z], down_ref.at[z], s)
        across(pair_place(s), down_out.at[s], d, s, start)
    finish_heads(heads, width, lam_ref, gain_ref, l_ref, acc_ref, out_ref)
    for d in range(nz):
        zz = lax.rem(z - d + nz, nz)
        for e in range(1, nx):
            arrived(pair_ref.at[z], down_ref.at[z], slot(zz, lax.rem(x - e + nx, nx)))
    for d in range(nz):
        zz = lax.rem(z - d + nz, nz)
        s = slot(zz, x)
        across(pair_place(s), down_out.at[s], d, s, sent)
        if d:
            along(d, sent)

    def settle(k, _):
        zz, _off = nearest(k, z, nz)
        flow(kv_ref, k, zz, sent)
        return 0

    lax.fori_loop(0, nz, settle, 0)


def gather_attend(nz, nx, queries, kv, lambdas, head_gain, pairs, downs):
    rows = queries.shape[0]
    heads = lambdas.shape[0]
    width = head_gain.shape[0]
    _, _, depth, mine = pairs.shape
    blocks = nz * nx
    vmem = pl.BlockSpec(memory_space=pltpu.VMEM)
    dma = pltpu.SemaphoreType.DMA
    side = max(nx - 1, 1)
    return pl.pallas_call(
        functools.partial(gather_attend_kernel, nz, nx, heads, 256),
        out_shape=[
            jax.ShapeDtypeStruct((rows, heads * width), jnp.bfloat16),
            jax.ShapeDtypeStruct((2, blocks * depth, mine), jnp.bfloat16),
            jax.ShapeDtypeStruct((blocks,) + downs.shape[1:], jnp.bfloat16),
        ],
        in_specs=[pl.BlockSpec(memory_space=pltpu.SMEM)] + [vmem] * 5,
        out_specs=[vmem] * 3,
        scratch_shapes=[pltpu.VMEM((blocks,) + kv.shape, jnp.bfloat16)]
        + [pltpu.VMEM((2 * heads, rows, width), jnp.float32)] * 3
        + [
            dma((nz,)), dma((nz,)), dma((side, nz)), dma((blocks,)),
            dma((nz,)), dma((nz,)), dma((side, nz)), dma((side, nz)), dma((blocks,)), dma((blocks,)),
        ],
        compiler_params=pltpu.CompilerParams(
            collective_id=0, has_side_effects=True, vmem_limit_bytes=60 * 1024 * 1024
        ),
        cost_estimate=pl.CostEstimate(
            flops=rows * rows * blocks * heads * 4096, bytes_accessed=4000000, transcendentals=0
        ),
        name="gather_attend",
    )(lambdas, queries, kv, head_gain.reshape(1, width), pairs, downs)


def per_device(
    nz, nx, residual, queries, key_pairs, values, lambdas, head_gain, w_out, norm_gain, w_gate, w_up, w_down
):
    local_rows = queries.shape[0]
    heads_here = lambdas.shape[0]
    value_width = head_gain.shape[0]
    d_rows, units = w_gate.shape
    mine = units // nz
    width = residual.shape[1]

    kv = jnp.concatenate([key_pairs, values], axis=1)
    pairs = jnp.stack([w_gate.reshape(d_rows, nz, mine), w_up.reshape(d_rows, nz, mine)], axis=2)
    pairs = jnp.transpose(pairs, (1, 2, 0, 3))
    heads_out, both, downs = gather_attend(
        nz, nx, queries, kv, lambdas, head_gain, pairs, w_down.reshape(nz, mine, w_down.shape[1])
    )
    gate, up = both[0], both[1]
    down = jnp.transpose(downs, (1, 0, 2)).reshape(mine, width)
    tp_index = lax.axis_index("tp")
    own_rows = local_rows // lax.axis_size("tp")
    w_mine = lax.dynamic_slice_in_dim(
        w_out, tp_index * heads_here * value_width, heads_here * value_width, 0
    )
    projected = lax.psum_scatter(
        jnp.dot(heads_out, w_mine, preferred_element_type=jnp.float32).astype(jnp.bfloat16),
        "tp",
        scatter_dimension=0,
        tiled=True,
    ).astype(jnp.float32)
    residual_own = lax.dynamic_slice_in_dim(residual, tp_index * own_rows, own_rows, 0)
    hidden_own = (residual_own.astype(jnp.float32) + projected).astype(jnp.bfloat16)
    stream_f = hidden_own.astype(jnp.float32)
    scaled = stream_f * lax.rsqrt(jnp.mean(stream_f * stream_f, axis=-1, keepdims=True) + 1e-05)
    normed_rows = lax.all_gather(
        (scaled * norm_gain).astype(jnp.bfloat16), ("z", "tp"), axis=0, tiled=True
    )
    gate_sum = jnp.dot(normed_rows, gate, preferred_element_type=jnp.float32)
    up_sum = jnp.dot(normed_rows, up, preferred_element_type=jnp.float32)
    hidden_units = (jax.nn.silu(gate_sum) * up_sum).astype(jnp.bfloat16)
    ffn_out = lax.psum_scatter(
        jnp.dot(hidden_units, down, preferred_element_type=jnp.float32).astype(jnp.bfloat16),
        ("z", "tp"),
        scatter_dimension=0,
        tiled=True,
    ).astype(jnp.float32)
    return (hidden_own.astype(jnp.float32) + ffn_out).astype(jnp.bfloat16)


def solution(mesh):
    sp, tp = mesh.shape["sp"], mesh.shape["tp"]
    coords = [getattr(d, "coords", None) for d in mesh.devices.flat]
    nx = len({c[0] for c in coords}) if all(c is not None for c in coords) else 2
    if sp % nx:
        nx = 1
    nz = sp // nx
    cube = Mesh(np.asarray(mesh.devices).reshape(nz, nx, tp), ("z", "x", "tp"))
    zx = ("z", "x")
    placed = (
        P(zx, None),
        P(zx, "tp"),
        P(zx, "tp"),
        P(zx, "tp"),
        P("tp"),
        P(),
        P(),
        P(),
        P(zx, "tp"),
        P(zx, "tp"),
        P("tp", zx),
    )
    return jax.shard_map(
        functools.partial(per_device, nz, nx),
        mesh=cube,
        in_specs=placed,
        out_specs=P(("z", "x", "tp"), None),
        check_vma=False,
    )
```

```python
import functools

import jax
import jax.numpy as jnp
import numpy as np
from jax import lax
from jax.experimental import pallas as pl
from jax.experimental.pallas import tpu as pltpu
from jax.sharding import Mesh, PartitionSpec as P

HD = 64


def attend_chunk(q, k, v, m_ref, l_ref, acc_ref, slot, rows):
    scores = lax.dot_general(
        q, k, (((1,), (1,)), ((), ())), preferred_element_type=jnp.float32
    )
    old = m_ref[slot, rows, :]
    high = jnp.maximum(old, jnp.max(scores, axis=1, keepdims=True))
    shrink = jnp.exp(old - high)
    weights = jnp.exp(scores - high[:, :1])
    l_ref[slot, rows, :] = l_ref[slot, rows, :] * shrink + jnp.sum(weights, axis=1, keepdims=True)
    m_ref[slot, rows, :] = high
    acc_ref[slot, rows, :] = acc_ref[slot, rows, :] * shrink + jnp.dot(
        weights.astype(jnp.bfloat16), v, preferred_element_type=jnp.float32
    )


def finish_heads(heads, width, lam_ref, gain_ref, l_ref, acc_ref, out_ref):
    for h in range(heads):
        first = acc_ref[2 * h] / l_ref[2 * h]
        second = acc_ref[2 * h + 1] / l_ref[2 * h + 1]
        differ = first - lam_ref[h] * second
        scale = lax.rsqrt(jnp.mean(differ * differ, axis=1, keepdims=True) + 1e-05)
        out_ref[:, h * width : (h + 1) * width] = (differ * scale * gain_ref[...]).astype(out_ref.dtype)


def nearest(k, me, n):
    low, high = me, n - 1 - me
    edge = jnp.minimum(low, high)
    side = jnp.where(high >= low, 1, -1)
    near = jnp.where(k % 2 == 1, 1, -1) * ((k + 1) // 2)
    off = side * jnp.where(k <= 2 * edge, near, k - edge)
    return me + off, off


def gather_attend_kernel(
    nz, nx, heads, block,
    lam_ref, q_ref, kv_ref, gain_ref, pair_ref, down_ref,
    out_ref, pair_out, down_out,
    kv_all, m_ref, l_ref, acc_ref,
    up_sem, low_sem, side_sem, kv_sem, pz_sem, dz_sem, px_sem, dx_sem, p_sem, d_sem,
):
    z, x = lax.axis_index("z"), lax.axis_index("x")
    rows_all = q_ref.shape[0]
    width = out_ref.shape[1] // heads
    keys = heads * 2 * HD
    depth = pair_ref.shape[2]

    def remote(src, dst, send, recv, zz, xx):
        return pltpu.make_async_remote_copy(
            src_ref=src, dst_ref=dst, send_sem=send, recv_sem=recv,
            device_id={"z": zz, "x": xx}, device_id_type=pl.DeviceIdType.MESH,
        )

    barrier = pltpu.get_barrier_semaphore()
    for a in range(nz):
        for b in range(nx):
            if a + b > 0:
                pl.semaphore_signal(
                    barrier, inc=1,
                    device_id={"z": lax.rem(z + a, nz), "x": lax.rem(x + b, nx)},
                    device_id_type=pl.DeviceIdType.MESH,
                )
    pl.semaphore_wait(barrier, nz * nx - 1)

    def slot(zz, xx):
        return zz * nx + xx

    def flow(src, k, zz, go):
        off = zz - z
        here = kv_all.at[slot(zz, x)]

        @pl.when(jnp.logical_and(off <= 0, z < nz - 1))
        def _():
            go(remote(src, here, up_sem.at[k], kv_sem.at[slot(zz, x)], jnp.minimum(z + 1, nz - 1), x))

        @pl.when(jnp.logical_and(off >= 0, z > 0))
        def _():
            go(remote(src, here, low_sem.at[k], kv_sem.at[slot(zz, x)], jnp.maximum(z - 1, 0), x))

        for e in range(1, nx):
            go(remote(src, here, side_sem.at[e - 1, k], kv_sem.at[slot(zz, x)], z, lax.rem(x + e, nx)))

    def pair_place(s):
        return pair_out.at[:, pl.ds(pl.multiple_of(s * depth, depth), depth), :]

    def along(d, go):
        to = lax.rem(z + d, nz)
        s = slot(z, x)
        go(remote(pair_ref.at[to], pair_place(s), pz_sem.at[d], p_sem.at[s], to, x))
        go(remote(down_ref.at[to], down_out.at[s], dz_sem.at[d], d_sem.at[s], to, x))

    def across(src_pair, src_down, d, s, go):
        for e in range(1, nx):
            to = lax.rem(x + e, nx)
            go(remote(src_pair, pair_place(s), px_sem.at[e - 1, d], p_sem.at[s], z, to))
            go(remote(src_down, down_out.at[s], dx_sem.at[e - 1, d], d_sem.at[s], z, to))

    def arrived(src_pair, src_down, s):
        remote(src_pair, pair_place(s), pz_sem.at[0], p_sem.at[s], z, x).wait_recv()
        remote(src_down, down_out.at[s], dz_sem.at[0], d_sem.at[s], z, x).wait_recv()

    start = lambda copy: copy.start()
    sent = lambda copy: copy.wait_send()

    flow(kv_ref, 0, z, start)
    mine = slot(z, x)
    pair_out[:, pl.ds(pl.multiple_of(mine * depth, depth), depth), :] = pair_ref[z]
    down_out[mine] = down_ref[z]
    kv_all[mine] = kv_ref[...]
    m_ref[...] = jnp.full_like(m_ref, -jnp.inf)
    l_ref[...] = jnp.zeros_like(l_ref)
    acc_ref[...] = jnp.zeros_like(acc_ref)

    def attend(s):
        for h in range(heads):
            v = kv_all[s, :, keys + h * width : keys + (h + 1) * width]
            for m in range(2):
                lane = (2 * h + m) * HD
                k = kv_all[s, :, lane : lane + HD]
                for r in range(0, rows_all, block):
                    rows = pl.ds(r, block)
                    q = q_ref[rows, lane : lane + HD] * jnp.bfloat16(HD**-0.5)
                    attend_chunk(q, k, v, m_ref, l_ref, acc_ref, 2 * h + m, rows)

    def step(k, _):
        zz, _off = nearest(k, z, nz)
        here = kv_all.at[slot(zz, x)]

        @pl.when(k > 0)
        def _():
            remote(kv_ref, here, up_sem.at[k], kv_sem.at[slot(zz, x)], z, x).wait_recv()
            flow(here, k, zz, start)

        @pl.when(k == min(1, nz - 1))
        def _():
            for d in range(1, nz):
                along(d, start)
            across(pair_ref.at[z], down_ref.at[z], 0, mine, start)

        def column(e, _):
            other = lax.rem(x - e + nx, nx)

            @pl.when(e > 0)
            def _():
                remote(kv_ref, here, up_sem.at[k], kv_sem.at[slot(zz, other)], z, x).wait_recv()

            attend(slot(zz, other))
            return 0

        lax.fori_loop(0, nx, column, 0)
        return 0

    lax.fori_loop(0, nz, step, 0)
    for d in range(1, nz):
        zz = lax.rem(z - d + nz, nz)
        s = slot(zz, x)
        arrived(pair_ref.at[z], down_ref.at[z], s)
        across(pair_place(s), down_out.at[s], d, s, start)
    finish_heads(heads, width, lam_ref, gain_ref, l_ref, acc_ref, out_ref)
    for d in range(nz):
        zz = lax.rem(z - d + nz, nz)
        for e in range(1, nx):
            arrived(pair_ref.at[z], down_ref.at[z], slot(zz, lax.rem(x - e + nx, nx)))
    for d in range(nz):
        zz = lax.rem(z - d + nz, nz)
        s = slot(zz, x)
        across(pair_place(s), down_out.at[s], d, s, sent)
        if d:
            along(d, sent)

    def settle(k, _):
        zz, _off = nearest(k, z, nz)
        flow(kv_ref, k, zz, sent)
        return 0

    lax.fori_loop(0, nz, settle, 0)


def gather_attend(nz, nx, queries, kv, lambdas, head_gain, pairs, downs):
    rows = queries.shape[0]
    heads = lambdas.shape[0]
    width = head_gain.shape[0]
    _, _, depth, mine = pairs.shape
    blocks = nz * nx
    vmem = pl.BlockSpec(memory_space=pltpu.VMEM)
    dma = pltpu.SemaphoreType.DMA
    side = max(nx - 1, 1)
    return pl.pallas_call(
        functools.partial(gather_attend_kernel, nz, nx, heads, 256),
        out_shape=[
            jax.ShapeDtypeStruct((rows, heads * width), jnp.bfloat16),
            jax.ShapeDtypeStruct((2, blocks * depth, mine), jnp.bfloat16),
            jax.ShapeDtypeStruct((blocks,) + downs.shape[1:], jnp.bfloat16),
        ],
        in_specs=[pl.BlockSpec(memory_space=pltpu.SMEM)] + [vmem] * 5,
        out_specs=[vmem] * 3,
        scratch_shapes=[pltpu.VMEM((blocks,) + kv.shape, jnp.bfloat16)]
        + [pltpu.VMEM((2 * heads, rows, width), jnp.float32)] * 3
        + [
            dma((nz,)), dma((nz,)), dma((side, nz)), dma((blocks,)),
            dma((nz,)), dma((nz,)), dma((side, nz)), dma((side, nz)), dma((blocks,)), dma((blocks,)),
        ],
        compiler_params=pltpu.CompilerParams(
            collective_id=0, has_side_effects=True, vmem_limit_bytes=60 * 1024 * 1024
        ),
        cost_estimate=pl.CostEstimate(
            flops=rows * rows * blocks * heads * 4096, bytes_accessed=4000000, transcendentals=0
        ),
        name="gather_attend",
    )(lambdas, queries, kv, head_gain.reshape(1, width), pairs, downs)


def gather_rows_kernel(nz, nt, own_ref, out_ref, up_sem, low_sem, y_sem, c_sem, got_sem):
    z, t = lax.axis_index("z"), lax.axis_index("tp")
    rows = own_ref.shape[0]
    partner = t + 1 - 2 * lax.rem(t, 2)

    barrier = pltpu.get_barrier_semaphore()
    for a in range(nz):
        for b in range(nt):
            if a + b > 0:
                pl.semaphore_signal(
                    barrier, inc=1,
                    device_id={"z": lax.rem(z + a, nz), "tp": lax.rem(t + b, nt)},
                    device_id_type=pl.DeviceIdType.MESH,
                )
    pl.semaphore_wait(barrier, nz * nt - 1)

    def place(zz, tt):
        s = zz * nt + tt
        return out_ref.at[pl.ds(pl.multiple_of(s * rows, rows), rows), :], got_sem.at[s]

    def remote(src, zz, tt, send, to_z, to_t):
        dst, recv = place(zz, tt)
        return pltpu.make_async_remote_copy(
            src_ref=src, dst_ref=dst, send_sem=send, recv_sem=recv,
            device_id={"z": to_z, "tp": to_t}, device_id_type=pl.DeviceIdType.MESH,
        )

    def flow(src, k, zz, go):
        @pl.when(jnp.logical_and(zz <= z, z < nz - 1))
        def _():
            go(remote(src, zz, t, up_sem.at[k], jnp.minimum(z + 1, nz - 1), t))

        @pl.when(jnp.logical_and(zz >= z, z > 0))
        def _():
            go(remote(src, zz, t, low_sem.at[k], jnp.maximum(z - 1, 0), t))

        for e in range(1, nt // 2):
            go(remote(src, zz, t, y_sem.at[k, e], z, lax.rem(t + 2 * e, nt)))
        go(remote(src, zz, t, c_sem.at[k, 0], z, partner))

    start = lambda copy: copy.start()
    sent = lambda copy: copy.wait_send()

    def await_block(zz, tt):
        remote(own_ref, zz, tt, c_sem.at[0, 0], z, partner).wait_recv()

    flow(own_ref, 0, z, start)
    mine, _sem = place(z, t)
    mine[...] = own_ref[...]

    def same_core(e):
        return lax.rem(t - 2 * e + nt, nt)

    def step(k, _):
        zz, _off = nearest(k, z, nz)

        @pl.when(k > 0)
        def _():
            await_block(zz, t)
            flow(place(zz, t)[0], k, zz, start)

        for e in range(1, nt // 2):
            tt = same_core(e)
            await_block(zz, tt)
            remote(place(zz, tt)[0], zz, tt, c_sem.at[k, e], z, partner).start()
        return 0

    lax.fori_loop(0, nz, step, 0)

    def settle(k, _):
        zz, _off = nearest(k, z, nz)
        flow(own_ref, k, zz, sent)
        for e in range(nt // 2):
            await_block(zz, lax.rem(partner - 2 * e + nt, nt))
            if e:
                tt = same_core(e)
                remote(own_ref, zz, tt, c_sem.at[k, e], z, partner).wait_send()
        return 0

    lax.fori_loop(0, nz, settle, 0)


def gather_rows(nz, nt, own):
    rows, width = own.shape
    if nt % 2:
        return lax.all_gather(own, ("z", "tp"), axis=0, tiled=True)
    vmem = pl.BlockSpec(memory_space=pltpu.VMEM)
    dma = pltpu.SemaphoreType.DMA
    return pl.pallas_call(
        functools.partial(gather_rows_kernel, nz, nt),
        out_shape=jax.ShapeDtypeStruct((nz * nt * rows, width), own.dtype),
        in_specs=[vmem],
        out_specs=vmem,
        scratch_shapes=[dma((nz,)), dma((nz,)), dma((nz, nt // 2)), dma((nz, nt // 2)), dma((nz * nt,))],
        compiler_params=pltpu.CompilerParams(
            collective_id=1, has_side_effects=True, vmem_limit_bytes=32 * 1024 * 1024
        ),
        cost_estimate=pl.CostEstimate(flops=10**10, bytes_accessed=4000000, transcendentals=0),
        name="gather_rows",
    )(own)


def per_device(
    nz, nx, residual, queries, key_pairs, values, lambdas, head_gain, w_out, norm_gain, w_gate, w_up, w_down
):
    local_rows = queries.shape[0]
    heads_here = lambdas.shape[0]
    value_width = head_gain.shape[0]
    d_rows, units = w_gate.shape
    mine = units // nz
    width = residual.shape[1]

    kv = jnp.concatenate([key_pairs, values], axis=1)
    pairs = jnp.stack([w_gate.reshape(d_rows, nz, mine), w_up.reshape(d_rows, nz, mine)], axis=2)
    pairs = jnp.transpose(pairs, (1, 2, 0, 3))
    heads_out, both, downs = gather_attend(
        nz, nx, queries, kv, lambdas, head_gain, pairs, w_down.reshape(nz, mine, w_down.shape[1])
    )
    gate, up = both[0], both[1]
    down = jnp.transpose(downs, (1, 0, 2)).reshape(mine, width)
    tp_index = lax.axis_index("tp")
    own_rows = local_rows // lax.axis_size("tp")
    w_mine = lax.dynamic_slice_in_dim(
        w_out, tp_index * heads_here * value_width, heads_here * value_width, 0
    )
    projected = lax.psum_scatter(
        jnp.dot(heads_out, w_mine, preferred_element_type=jnp.float32).astype(jnp.bfloat16),
        "tp",
        scatter_dimension=0,
        tiled=True,
    ).astype(jnp.float32)
    residual_own = lax.dynamic_slice_in_dim(residual, tp_index * own_rows, own_rows, 0)
    hidden_own = (residual_own.astype(jnp.float32) + projected).astype(jnp.bfloat16)
    stream_f = hidden_own.astype(jnp.float32)
    scaled = stream_f * lax.rsqrt(jnp.mean(stream_f * stream_f, axis=-1, keepdims=True) + 1e-05)
    normed_rows = gather_rows(nz, lax.axis_size("tp"), (scaled * norm_gain).astype(jnp.bfloat16))
    gate_sum = jnp.dot(normed_rows, gate, preferred_element_type=jnp.float32)
    up_sum = jnp.dot(normed_rows, up, preferred_element_type=jnp.float32)
    hidden_units = (jax.nn.silu(gate_sum) * up_sum).astype(jnp.bfloat16)
    ffn_out = lax.psum_scatter(
        jnp.dot(hidden_units, down, preferred_element_type=jnp.float32).astype(jnp.bfloat16),
        ("z", "tp"),
        scatter_dimension=0,
        tiled=True,
    ).astype(jnp.float32)
    return (hidden_own.astype(jnp.float32) + ffn_out).astype(jnp.bfloat16)


def solution(mesh):
    sp, tp = mesh.shape["sp"], mesh.shape["tp"]
    coords = [getattr(d, "coords", None) for d in mesh.devices.flat]
    nx = len({c[0] for c in coords}) if all(c is not None for c in coords) else 2
    if sp % nx:
        nx = 1
    nz = sp // nx
    cube = Mesh(np.asarray(mesh.devices).reshape(nz, nx, tp), ("z", "x", "tp"))
    zx = ("z", "x")
    placed = (
        P(zx, None),
        P(zx, "tp"),
        P(zx, "tp"),
        P(zx, "tp"),
        P("tp"),
        P(),
        P(),
        P(),
        P(zx, "tp"),
        P(zx, "tp"),
        P("tp", zx),
    )
    return jax.shard_map(
        functools.partial(per_device, nz, nx),
        mesh=cube,
        in_specs=placed,
        out_specs=P(("z", "x", "tp"), None),
        check_vma=False,
    )
```
